32 devices in a mesh: sp: 16 (over z, y, x), tp: 2 (over core).
Axes of the slice: x: 2, y: 2, z: 4, core: 2. Of those that a mesh axis runs over, the one named last changes fastest.
Arguments:
- tokens: bfloat16 [8192, 2048], P(('sp', 'tp')), may hold values from -6 to 6
- norm_gain: float32 [2048], replicated, may hold values from 0.1 to 1.9
- in_weight: bfloat16 [2048, 1024], P(None, 'tp'), may hold values from -0.125 to 0.125
- gate_weight: bfloat16 [2048, 1024], P(None, 'tp'), may hold values from -0.125 to 0.125
- conv_weight: float32 [4, 1024], P(None, 'tp'), may hold values from -3 to 3
- decay_gate_weight: bfloat16 [16, 64, 64], P('tp'), may hold values from -0.75 to 0.75
- decay_gate_bias: float32 [1024], P('tp'), may hold values from -4 to 4
- input_gate_weight: bfloat16 [16, 64, 64], P('tp'), may hold values from -0.75 to 0.75
- input_gate_bias: float32 [1024], P('tp'), may hold values from -4 to 4
- channel_decay_rate: float32 [1024], P('tp'), may hold values from 4.8828125e-06 to 0.01
- forgetting_offset: float32 [16, 8192], P('tp', 'sp'), may hold values from -1.6 to 0
- out_weight: bfloat16 [1024, 2048], P('tp'), may hold values from -0.1875 to 0.1875
Outputs:
- mixed: bfloat16 [8192, 2048], P(('sp', 'tp'))
The draws below stay inside these ranges and needn't reach their ends.
All inputs are finite; a program needn't handle non-finite values.
Results may differ from the reference program's by a relative error of at most 0.0067.
Values may be sent and summed in bfloat16 or wider, within the bound.
A program may use at most 64 MiB of HBM per device.

```python
import math
import jax
import jax.numpy as jnp
from jax import lax

D = 2048
HEADS = 16
BLOCK = 64
CONV = 4
TOK_DEV = 256
WIDTH = 1024
GROUP = 512
TOKENS = 8192
N_SP = 16
N_TP = 2


def draw_channel_decay_rate(key, part):
    width = HEADS * BLOCK
    key_pick = jax.random.fold_in(key, 11)
    key_fast = jax.random.fold_in(key, 12)
    key_slow = jax.random.fold_in(key, 13)
    share = 50
    picked = jax.random.randint(key_pick, (width,), 0, 100) < share
    fast_rate = jnp.exp(jax.random.uniform(key_fast, (width,), jnp.float32, math.log(0.003), math.log(0.01)))
    slow_rate = jnp.exp(jax.random.uniform(key_slow, (width,), jnp.float32, math.log(0.04), math.log(0.08))) / TOKENS
    return jnp.where(picked, fast_rate, slow_rate).astype(jnp.float32)


def draw_forgetting_offset(key, part):
    count = TOKENS // GROUP
    key_factor = jax.random.fold_in(key, 21)
    key_spot = jax.random.fold_in(key, 22)
    key_loss = jax.random.fold_in(key, 23)
    factor = jnp.exp(jax.random.uniform(key_factor, (HEADS, count), jnp.float32, 0.0, math.log(4.0)))
    steady_threshold = -(0.2 / TOKENS) * jnp.repeat(factor, GROUP, axis=1)
    spots = jax.random.randint(key_spot, (HEADS, 3, 1), 0, TOKENS)
    objective_terms = jax.random.uniform(key_loss, (HEADS, 3, 1), jnp.float32, 0.22, 0.5)
    assigned_locations = jnp.arange(TOKENS, dtype=jnp.int32)[None, None, :] == spots
    contiguous_intervals = jnp.sum(jnp.where(assigned_locations, -objective_terms, 0.0), axis=1)
    return (steady_threshold + contiguous_intervals).astype(jnp.float32)


def levels(own_key, extent, cuts, smallest, largest):
    factor_of, own = 1.0, jax.random.fold_in(own_key, 6)
    for position, parts in cuts:
        steps = jnp.exp(jax.random.uniform(jax.random.fold_in(own, position), (parts,), jnp.float32, smallest / len(cuts), largest / len(cuts)))
        factor_of = factor_of * jnp.repeat(steps, extent[position] // parts).reshape([-1 if axis == position else 1 for axis in range(len(extent))])
    return factor_of


def noise(key, shape, deviation, bound, shards=(), held_as=jnp.bfloat16):
    loudness = levels(key, shape, shards, -0.22, 0.18) if shards else 1.0
    drawn = jax.random.normal(key, shape, jnp.float32) * deviation * loudness
    return jnp.minimum(jnp.maximum(drawn, -bound), bound).astype(held_as)


def setup_inputs(seed: int = 0) -> dict:
    key_list = jax.random.split(jax.random.key(seed), 13)
    tokens = noise(key_list[0], (TOKENS, D), 1.0, 6.0, ((0, 32),))
    norm_gain = jnp.clip(1.0 + 0.18 * jax.random.normal(key_list[1], (D,), jnp.float32), 0.1, 1.9)
    in_weight = noise(key_list[2], (D, WIDTH), D ** -0.5, 0.125, ((1, 2),))
    gate_weight = noise(key_list[3], (D, WIDTH), D ** -0.5, 0.125, ((1, 2),))
    conv_weight = noise(key_list[4], (CONV, WIDTH), CONV ** -0.5, 3.0, ((1, 2),), jnp.float32)
    decay_gate_weight = noise(key_list[5], (HEADS, BLOCK, BLOCK), BLOCK ** -0.5, 0.75, ((0, 2),))
    decay_gate_bias = noise(key_list[6], (WIDTH,), 1.0, 4.0, ((0, 2),), jnp.float32)
    input_gate_weight = noise(key_list[7], (HEADS, BLOCK, BLOCK), BLOCK ** -0.5, 0.75, ((0, 2),))
    input_gate_bias = noise(key_list[8], (WIDTH,), 1.0, 4.0, ((0, 2),), jnp.float32)
    channel_decay_rate = draw_channel_decay_rate(jax.random.fold_in(key_list[12], 71), 0)
    forgetting_offset = draw_forgetting_offset(jax.random.fold_in(key_list[12], 71), 0)
    out_weight = noise(key_list[11], (WIDTH, D), WIDTH ** -0.5, 0.1875, ((0, 2),))
    return {"tokens": tokens, "norm_gain": norm_gain, "in_weight": in_weight, "gate_weight": gate_weight, "conv_weight": conv_weight, "decay_gate_weight": decay_gate_weight, "decay_gate_bias": decay_gate_bias, "input_gate_weight": input_gate_weight, "input_gate_bias": input_gate_bias, "channel_decay_rate": channel_decay_rate, "forgetting_offset": forgetting_offset, "out_weight": out_weight}


epsilon = 1e-05

def link(earlier, later):
    return (earlier[0] * later[0], later[0] * earlier[1] + later[1])

def reference(tokens, norm_gain, in_weight, gate_weight, conv_weight, decay_gate_weight, decay_gate_bias, input_gate_weight, input_gate_bias, channel_decay_rate, forgetting_offset, out_weight):
    length = TOK_DEV * N_TP
    count = N_SP
    width = HEADS * BLOCK
    token_blocks = tokens.reshape(count, length, D)
    shift_blocks = forgetting_offset.reshape(HEADS, count, length).transpose(1, 2, 0)

    def advance(carry, item):
        prior, tail = carry
        interval_matrix_lines, shift_rows = item
        floats = interval_matrix_lines.astype(jnp.float32)
        middle_point = floats - lax.optimization_barrier(jnp.mean(floats, axis=1, keepdims=True))
        spread = lax.optimization_barrier(jnp.mean(middle_point * middle_point, axis=1, keepdims=True))
        normed = (middle_point * lax.rsqrt(spread + epsilon) * norm_gain).astype(jnp.bfloat16)
        inner = jnp.dot(normed, in_weight, preferred_element_type=jnp.float32).astype(jnp.bfloat16)
        gate = jnp.dot(normed, gate_weight, preferred_element_type=jnp.float32).astype(jnp.bfloat16)
        extended = jnp.concatenate([tail, inner], axis=0)
        smooth = extended[0:length].astype(jnp.float32) * conv_weight[0]
        for tap in range(1, CONV):
            smooth = smooth + extended[tap:tap + length].astype(jnp.float32) * conv_weight[tap]
        smoothed = smooth.astype(jnp.bfloat16)
        grouped = smoothed.astype(jnp.float32).reshape(length, HEADS, BLOCK)
        retain = jax.nn.sigmoid(jnp.einsum('rhi,hij->rhj', grouped, decay_gate_weight.astype(jnp.float32)).reshape(length, width) + decay_gate_bias)
        admit = jax.nn.sigmoid(jnp.einsum('rhi,hij->rhj', grouped, input_gate_weight.astype(jnp.float32)).reshape(length, width) + input_gate_bias)
        log_decay = -8.0 * retain * channel_decay_rate + jnp.repeat(shift_rows, BLOCK, axis=1)
        decay = jnp.exp(log_decay)
        drive = jnp.sqrt(-jnp.expm1(2.0 * log_decay)) * admit * smoothed.astype(jnp.float32)
        product, local = lax.associative_scan(link, (decay, drive), axis=0)
        state = local + product * prior
        gated = (state * jax.nn.gelu(gate.astype(jnp.float32))).astype(jnp.bfloat16)
        result = jnp.dot(gated, out_weight, preferred_element_type=jnp.float32).astype(jnp.bfloat16)
        return ((state[length - 1], inner[length - CONV + 1:]), result)
    start = (jnp.zeros((width,), jnp.float32), jnp.zeros((CONV - 1, width), jnp.bfloat16))
    _, results = lax.scan(advance, start, (token_blocks, shift_blocks))
    return results.reshape(TOKENS, D)
```

```python
import functools

import jax
import jax.numpy as jnp
from jax import lax
from jax.experimental import pallas as pl
from jax.experimental.pallas import tpu as pltpu
from jax.sharding import PartitionSpec as P

epsilon = 1e-05


def from_behind(value, axis, steps):
    count = lax.axis_size(axis)
    first, last = (max(0, -steps), min(count, count - steps))
    return lax.ppermute(value, axis, [(source, source + steps) for source in range(first, last)])


LANES = 128
PIECES = 8


def scan_kernel(decay_ref, drive_ref, ends_ref, local_ref, product_ref):
    steps = decay_ref.shape[0] // PIECES

    def one(j, carry):
        p, h = carry
        rows = pl.ds(j, PIECES, stride=steps)
        a = decay_ref[rows, :]
        h = a * h + drive_ref[rows, :]
        p = a * p
        local_ref[rows, :] = h
        product_ref[rows, :] = p
        return p, h

    zero = jnp.zeros((PIECES, LANES), jnp.float32)
    p, h = lax.fori_loop(0, steps, one, (zero + 1.0, zero), unroll=8)
    before_h = h[0:1]
    before_p = p[0:1]
    for piece in range(1, PIECES):
        rows = pl.ds(piece * steps, steps)
        part = product_ref[rows, :]
        local_ref[rows, :] = local_ref[rows, :] + part * before_h
        product_ref[rows, :] = part * before_p
        before_h = p[piece : piece + 1] * before_h + h[piece : piece + 1]
        before_p = p[piece : piece + 1] * before_p
    ends_ref[0:1, :] = before_p
    ends_ref[1:2, :] = before_h


def local_scan(decay, drive):
    length, width = decay.shape
    block = pl.BlockSpec((length, LANES), lambda i: (0, i))
    whole = jax.ShapeDtypeStruct((length, width), jnp.float32)
    return pl.pallas_call(
        scan_kernel,
        grid=(width // LANES,),
        in_specs=[block, block],
        out_specs=[pl.BlockSpec((2, LANES), lambda i: (0, i)), block, block],
        out_shape=[jax.ShapeDtypeStruct((2, width), jnp.float32), whole, whole],
        name="local_scan",
    )(decay, drive)


def prefix_kernel(count, ends_ref, carry_ref, slots, send_sem, recv_sem):
    me = lax.axis_index("sp")
    barrier = pltpu.get_barrier_semaphore()

    def greet(k, _):
        pl.semaphore_signal(
            barrier,
            inc=1,
            device_id={"sp": lax.rem(me + k, count)},
            device_id_type=pl.DeviceIdType.MESH,
        )
        return 0

    lax.fori_loop(1, count, greet, 0)
    pl.semaphore_wait(barrier, count - 1)

    def copy(source, target):
        return pltpu.make_async_remote_copy(
            src_ref=ends_ref,
            dst_ref=slots.at[source],
            send_sem=send_sem.at[target],
            recv_sem=recv_sem.at[source],
            device_id={"sp": target},
            device_id_type=pl.DeviceIdType.MESH,
        )

    def send(target, _):
        copy(me, target).start()
        return 0

    lax.fori_loop(me + 1, count, send, 0)
    carry_ref[...] = jnp.zeros_like(carry_ref)

    def receive(source, _):
        copy(source, me).wait_recv()
        carry_ref[...] = slots[source, 0:1, :] * carry_ref[...] + slots[source, 1:2, :]
        return 0

    lax.fori_loop(0, me, receive, 0)

    def sent(target, _):
        copy(me, target).wait_send()
        return 0

    lax.fori_loop(me + 1, count, sent, 0)


def prefix(ends):
    count = lax.axis_size("sp")
    width = ends.shape[1]
    return pl.pallas_call(
        functools.partial(prefix_kernel, count),
        in_specs=[pl.BlockSpec(memory_space=pltpu.VMEM)],
        out_specs=pl.BlockSpec(memory_space=pltpu.VMEM),
        out_shape=jax.ShapeDtypeStruct((1, width), jnp.float32),
        scratch_shapes=[
            pltpu.VMEM((count, 2, width), jnp.float32),
            pltpu.SemaphoreType.DMA((count,)),
            pltpu.SemaphoreType.DMA((count,)),
        ],
        compiler_params=pltpu.CompilerParams(collective_id=0, has_side_effects=True),
        name="prefix",
    )(ends)


def body(
    tokens,
    norm_gain,
    in_weight,
    gate_weight,
    conv_weight,
    decay_gate_weight,
    decay_gate_bias,
    input_gate_weight,
    input_gate_bias,
    channel_decay_rate,
    forgetting_offset,
    out_weight,
):
    floats = tokens.astype(jnp.float32)
    middle_point = floats - jnp.mean(floats, axis=1, keepdims=True)
    spread = jnp.mean(middle_point * middle_point, axis=1, keepdims=True)
    normed = (middle_point * lax.rsqrt(spread + epsilon) * norm_gain).astype(jnp.bfloat16)
    joined = jnp.concatenate([in_weight, gate_weight], axis=1)
    width = in_weight.shape[1]
    projected = jnp.dot(
        lax.all_gather(normed, "tp", axis=0, tiled=True), joined, preferred_element_type=jnp.float32
    ).astype(jnp.bfloat16)
    inner = projected[:, :width]
    gate = projected[:, width:]
    length = inner.shape[0]
    taps = conv_weight.shape[0]
    before = from_behind(inner[length - taps + 1 :], "sp", 1)
    extended = jnp.concatenate([before, inner], axis=0)
    smooth = extended[0:length].astype(jnp.float32) * conv_weight[0]
    for tap in range(1, taps):
        smooth = smooth + extended[tap : tap + length].astype(jnp.float32) * conv_weight[tap]
    smoothed = smooth.astype(jnp.bfloat16)
    heads = decay_gate_weight.shape[0]
    block = decay_gate_weight.shape[1]
    grouped = smoothed.reshape(length, heads, block)
    retain = jax.nn.sigmoid(
        jnp.einsum(
            "rhi,hij->rhj", grouped, decay_gate_weight, preferred_element_type=jnp.float32
        ).reshape(length, width)
        + decay_gate_bias
    )
    admit = jax.nn.sigmoid(
        jnp.einsum(
            "rhi,hij->rhj", grouped, input_gate_weight, preferred_element_type=jnp.float32
        ).reshape(length, width)
        + input_gate_bias
    )
    log_decay = -8.0 * retain * channel_decay_rate + jnp.repeat(forgetting_offset.T, block, axis=1)
    decay = jnp.exp(log_decay)
    drive = jnp.sqrt(-jnp.expm1(2.0 * log_decay)) * admit * smoothed.astype(jnp.float32)
    ends, local, product = local_scan(decay, drive)
    state = local + product * prefix(ends)
    gated = (state * jax.nn.gelu(gate.astype(jnp.float32))).astype(jnp.bfloat16)
    by_token = lax.all_to_all(gated, "tp", split_axis=0, concat_axis=1, tiled=True)
    full_rows = lax.all_gather(out_weight, "tp", axis=0, tiled=True)
    result = jnp.dot(by_token, full_rows, preferred_element_type=jnp.float32)
    return result.astype(jnp.bfloat16)


def solution(mesh):
    placed = (
        P(("sp", "tp"), None),
        P(),
        P(None, "tp"),
        P(None, "tp"),
        P(None, "tp"),
        P("tp", None, None),
        P("tp"),
        P("tp", None, None),
        P("tp"),
        P("tp"),
        P("tp", "sp"),
        P("tp", None),
    )
    return jax.shard_map(
        body, mesh=mesh, in_specs=placed, out_specs=P(("sp", "tp"), None), check_vma=False
    )
```
